32 devices in a mesh: grp: 1, ep: 32 (over z, y, x, core).
Axes of the slice: x: 2, y: 2, z: 4, core: 2. Of those that a mesh axis runs over, the one named last changes fastest.
Arguments:
- residual_input: bfloat16 [768, 2048], P(('grp', 'ep')), may hold values from -6 to 6
- attention_norm_gain: bfloat16 [2048], replicated, may hold values from 0.099609375 to 1.8984375
- receptance_weight: bfloat16 [2048, 1024], P(None, 'ep'), may hold values from -0.125 to 0.125
- key_weight: bfloat16 [2048, 1024], P(None, 'ep'), may hold values from -0.125 to 0.125
- value_weight: bfloat16 [2048, 1024], P(None, 'ep'), may hold values from -0.125 to 0.125
- decay_weight: bfloat16 [2048, 1024], P(None, 'ep'), may hold values from -0.125 to 0.125
- correction_rate_weight: bfloat16 [2048, 1024], P(None, 'ep'), may hold values from -0.125 to 0.125
- output_gate_weight: bfloat16 [2048, 1024], P(None, 'ep'), may hold values from -0.125 to 0.125
- decay_offset: float32 [1024], replicated, may hold values from -3 to 1
- correction_rate_offset: float32 [1024], replicated, may hold values from -1.5 to 1.5
- self_term_weight: float32 [1024], replicated, may hold values from -2 to 2
- head_read_gain: float32 [1024], replicated, may hold values from 0.1 to 1.9
- previous_state: float32 [768, 16, 4096], P(('grp', 'ep')), may hold values from -4 to 4
- attention_output_weight: bfloat16 [1024, 2048], replicated, may hold values from -0.1875 to 0.1875
- feedforward_norm_gain: bfloat16 [2048], replicated, may hold values from 0.099609375 to 1.8984375
- routes: int32 [768, 4], P('grp'), may hold values from 0 to 31, all different within a row; in each aligned block of 24 rows (0 to 23, 24 to 47, ...) at most 4 rows name the same one
- routing_weight: float32 [768, 4], P('grp'), may hold values from 0.2 to 1
- routed_gate_weight: bfloat16 [32, 2048, 512], P('ep'), may hold values from -0.125 to 0.125
- routed_up_weight: bfloat16 [32, 2048, 512], P('ep'), may hold values from -0.125 to 0.125
- routed_down_weight: bfloat16 [32, 512, 2048], P('ep'), may hold values from -0.25 to 0.25
- common_gate_weight: bfloat16 [2048, 512], replicated, may hold values from -0.125 to 0.125
- common_up_weight: bfloat16 [2048, 512], replicated, may hold values from -0.125 to 0.125
- common_down_weight: bfloat16 [512, 2048], replicated, may hold values from -0.25 to 0.25
Outputs:
- hidden_out: bfloat16 [768, 2048], P(('grp', 'ep'))
- next_state: float32 [768, 16, 4096], P(('grp', 'ep'))
The draws below stay inside these ranges and needn't reach their ends.
Inputs may be any that keep to these rules, and one draw needn't show every extreme that they name: `routes`: the 4 entries of a row differ. In each aligned block of 24 rows (the tokens of one index of ep) no expert is named by more than 4 rows, a bound that some block reaches.
All inputs are finite; a program needn't handle non-finite values.
Results may differ from the reference program's by a relative error of at most 0.013.
Values may be sent and summed in bfloat16 or wider, within the bound.
No kernel may reach another device: no remote copies, remote signals or barrier semaphores. Data moves between devices by JAX's collectives and lax.ppermute only.
A program may use at most 128 MiB of HBM per device.

```python
import math
import jax
import jax.numpy as jnp
import numpy as np
from jax import lax

D = 2048
HEAD_COUNT = 16
HEAD_SIZE = 64
MIXER_WIDTH = 1024
EFF = 512
SFF = 512
EXPERTS = 32
TOPK = 4
CAP = 4
SEQ_DEV = 24
TOKENS = 768
N_EP = 32


def block_levels(key, shape, shards, least, high):
    level, own = 1.0, jax.random.fold_in(key, 6)
    for position, blocks in shards:
        heights = jnp.exp(jax.random.uniform(jax.random.fold_in(own, position), (blocks,), jnp.float32, least / len(shards), high / len(shards)))
        level = level * jnp.repeat(heights, shape[position] // blocks).reshape([-1 if axis == position else 1 for axis in range(len(shape))])
    return level


def routed_block(key, own, number, rows, amount, top, reach, skew):
    sequence = jax.random.permutation(key, amount)
    heavy_load, common = shares(amount, rows * top, reach, skew, True), shares(amount, rows * top, reach, skew, False)
    places = jnp.arange(amount)

    def named(tallies, turn):
        used = int((tallies > 0).sum())
        fixed = max(1, used // 4)
        passed = fixed + (places - fixed + turn * (used - fixed)) % max(1, amount - fixed)
        return jnp.zeros((amount,), jnp.int32).at[sequence[jnp.where(places < fixed, places, passed)]].set(jnp.asarray(tallies, jnp.int32))

    tallies = jnp.where(number % 4 == 0, named(heavy_load, number // 4), named(common, number - number // 4 - 1))
    mixed = jax.random.permutation(jax.random.fold_in(own, 3), amount)
    source_of, receiver = mixed[0:amount // 2 * 2:2], mixed[1:amount // 2 * 2:2]
    room = jnp.minimum(tallies[source_of] - 1, reach - tallies[receiver]) // 2
    room = jnp.where((source_of == sequence[0]) | (receiver == sequence[0]) | (tallies[receiver] == 0), 0, jnp.maximum(room, 0))
    passed = jax.random.randint(jax.random.fold_in(own, 4), (amount // 2,), 0, 1 << 20) % (room + 1)
    tallies = tallies.at[source_of].add(-passed).at[receiver].add(passed)
    members = jnp.searchsorted(jnp.cumsum(tallies), jnp.arange(rows * top), side="right").astype(jnp.int32)
    table = members.reshape(top, rows).T
    table = table[jax.random.permutation(jax.random.fold_in(own, 1), rows)]
    turn = jax.random.randint(jax.random.fold_in(own, 2), (rows, 1), 0, top)
    return jnp.take_along_axis(table, (jnp.arange(top)[None, :] + turn) % top, axis=1)


def shares(count, total, most, slope, full):
    loads = [(1 << 20) // math.isqrt(rank ** slope) + 1 for rank in range(1, count + 1)]
    largest = most if full else min(most, max(-(-total // count), total * loads[0] // sum(loads)))
    least = 1 if total - largest >= count - 1 else 0
    given, rest = [largest] + [least] * (count - 1), total - largest - least * (count - 1)
    while rest > 0:
        candidates = [i for i in range(1, count) if given[i] < largest] or [i for i in range(1, count) if given[i] < most]
        mass, remaining = sum([loads[i] for i in candidates]), rest
        for i in candidates:
            extra = min(most - given[i], max(1, remaining * loads[i] // mass), rest)
            given[i] = given[i] + extra
            rest = rest - extra
    return np.array(given)


def scatter_about(own_key, dims, scale, most, shards=(), kind=jnp.bfloat16):
    level = block_levels(own_key, dims, shards, -0.22, 0.18) if shards else 1.0
    drawn = jax.random.normal(own_key, dims, jnp.float32) * scale * level
    return jnp.minimum(jnp.maximum(drawn, -most), most).astype(kind)


def setup_inputs(seed: int = 0, part: int = 0) -> dict:
    splits = jax.random.split(jax.random.key(seed), 24)
    part_keys = jax.random.split(jax.random.fold_in(splits[23], part), 24)
    residual_input = scatter_about(part_keys[0], (TOKENS, D), 1.0, 6.0, ((0, 32),))
    attention_norm_gain = jnp.clip(1.0 + 0.18 * jax.random.normal(splits[1], (D,), jnp.float32), 0.099609375, 1.8984375).astype(jnp.bfloat16)
    receptance_weight = scatter_about(splits[2], (D, MIXER_WIDTH), D ** -0.5, 0.125, ((1, 32),))
    key_weight = scatter_about(splits[3], (D, MIXER_WIDTH), D ** -0.5, 0.125, ((1, 32),))
    value_weight = scatter_about(splits[4], (D, MIXER_WIDTH), D ** -0.5, 0.125, ((1, 32),))
    decay_weight = scatter_about(splits[5], (D, MIXER_WIDTH), D ** -0.5, 0.125, ((1, 32),))
    correction_rate_weight = scatter_about(splits[6], (D, MIXER_WIDTH), D ** -0.5, 0.125, ((1, 32),))
    output_gate_weight = scatter_about(splits[7], (D, MIXER_WIDTH), D ** -0.5, 0.125, ((1, 32),))
    decay_offset = jnp.clip(jax.random.uniform(splits[8], (MIXER_WIDTH,), jnp.float32, -3.0, 1.0), -3.0, 1.0)
    correction_rate_offset = jnp.clip(jax.random.uniform(splits[9], (MIXER_WIDTH,), jnp.float32, -1.5, 1.5), -1.5, 1.5)
    self_term_weight = scatter_about(splits[10], (MIXER_WIDTH,), 0.15, 2.0, (), jnp.float32)
    head_read_gain = jnp.clip(1.0 + 0.18 * jax.random.normal(splits[11], (MIXER_WIDTH,), jnp.float32), 0.1, 1.9)
    previous_state = scatter_about(part_keys[12], (TOKENS, HEAD_COUNT, HEAD_SIZE * HEAD_SIZE), 0.3, 4.0, ((0, 32),), jnp.float32)
    attention_output_weight = scatter_about(splits[13], (MIXER_WIDTH, D), MIXER_WIDTH ** -0.5, 0.1875)
    feedforward_norm_gain = jnp.clip(1.0 + 0.18 * jax.random.normal(splits[14], (D,), jnp.float32), 0.099609375, 1.8984375).astype(jnp.bfloat16)
    routes_keys = jax.random.split(jax.random.fold_in(part_keys[15], 1), TOKENS // SEQ_DEV)
    routes_turns = jax.random.permutation(jax.random.fold_in(part_keys[15], 3), TOKENS // SEQ_DEV)
    routes = jax.vmap(lambda own, number: routed_block(jax.random.fold_in(part_keys[15], 2), own, number, SEQ_DEV, EXPERTS, TOPK, CAP, 2))(routes_keys, routes_turns).reshape((TOKENS, TOPK))
    routing_weight = jnp.clip(jax.random.uniform(part_keys[16], (TOKENS, TOPK), jnp.float32, 0.2, 1.0), 0.2, 1.0)
    routed_gate_weight = scatter_about(splits[17], (EXPERTS, D, EFF), D ** -0.5, 0.125, ((0, 32),))
    routed_up_weight = scatter_about(splits[18], (EXPERTS, D, EFF), D ** -0.5, 0.125, ((0, 32),))
    routed_down_weight = scatter_about(splits[19], (EXPERTS, EFF, D), EFF ** -0.5, 0.25, ((0, 32),))
    common_gate_weight = scatter_about(splits[20], (D, SFF), D ** -0.5, 0.125)
    common_up_weight = scatter_about(splits[21], (D, SFF), D ** -0.5, 0.125)
    common_down_weight = scatter_about(splits[22], (SFF, D), SFF ** -0.5, 0.25)
    return {"residual_input": residual_input, "attention_norm_gain": attention_norm_gain, "receptance_weight": receptance_weight, "key_weight": key_weight, "value_weight": value_weight, "decay_weight": decay_weight, "correction_rate_weight": correction_rate_weight, "output_gate_weight": output_gate_weight, "decay_offset": decay_offset, "correction_rate_offset": correction_rate_offset, "self_term_weight": self_term_weight, "head_read_gain": head_read_gain, "previous_state": previous_state, "attention_output_weight": attention_output_weight, "feedforward_norm_gain": feedforward_norm_gain, "routes": routes, "routing_weight": routing_weight, "routed_gate_weight": routed_gate_weight, "routed_up_weight": routed_up_weight, "routed_down_weight": routed_down_weight, "common_gate_weight": common_gate_weight, "common_up_weight": common_up_weight, "common_down_weight": common_down_weight}


def rms_norm(value_rows, gain):
    scale = lax.rsqrt(lax.optimization_barrier(jnp.mean(value_rows * value_rows, axis=-1, keepdims=True)) + 1e-06)
    return (value_rows * scale * gain.astype(jnp.float32)).astype(jnp.bfloat16)

def expert_mlp(rows, gate_w, up_w, down_w):
    gate = jnp.dot(rows, gate_w, preferred_element_type=jnp.float32)
    upward = jnp.dot(rows, up_w, preferred_element_type=jnp.float32)
    hidden = (jax.nn.silu(gate) * upward).astype(jnp.bfloat16)
    return jnp.dot(hidden, down_w, preferred_element_type=jnp.float32).astype(jnp.bfloat16)

def attention_mixer(receptance_rows, key_rows, value_rows, decay_logit, rate_logit, gate_logit, decay_offset, correction_rate_offset, self_term_weight, head_read_gain, head_state):
    tally_value = receptance_rows.shape[0]

    def heads(tensor):
        return tensor.astype(jnp.float32).reshape(tally_value, HEAD_COUNT, HEAD_SIZE)
    decay = jnp.exp(-jnp.exp(-jax.nn.softplus(-(decay_offset + decay_logit.astype(jnp.float32))) - 0.5))
    rate = jax.nn.sigmoid(correction_rate_offset + rate_logit.astype(jnp.float32))
    key_head = heads(key_rows)
    rate_head = heads(rate)
    receptance_head = heads(receptance_rows)
    head_value = heads(value_rows)
    unit_key = key_head * lax.rsqrt(1.0 + lax.optimization_barrier(jnp.sum(key_head * key_head, axis=-1, keepdims=True)))
    rate_scaled_key = key_head * rate_head
    removal = unit_key * rate_head
    matrix = head_state.reshape(tally_value, HEAD_COUNT, HEAD_SIZE, HEAD_SIZE)
    recalled = jnp.einsum('nhvk,nhk->nhv', matrix, unit_key, precision=lax.Precision.HIGHEST)
    matrix = matrix * heads(decay)[:, :, None, :] - recalled[..., None] * removal[:, :, None, :] + head_value[..., None] * rate_scaled_key[:, :, None, :]
    read = jnp.einsum('nhvk,nhk->nhv', matrix, receptance_head, precision=lax.Precision.HIGHEST)
    centered = read - lax.optimization_barrier(jnp.mean(read, axis=-1, keepdims=True))
    variance = lax.optimization_barrier(jnp.mean(centered * centered, axis=-1, keepdims=True))
    normed_head_read = centered * lax.rsqrt(variance + 0.00064) * head_read_gain.reshape(HEAD_COUNT, HEAD_SIZE)
    self_term = lax.optimization_barrier(jnp.sum(receptance_head * rate_scaled_key * self_term_weight.reshape(HEAD_COUNT, HEAD_SIZE), axis=-1, keepdims=True)) * head_value
    normed_mixer_input = (normed_head_read + self_term).reshape(tally_value, HEAD_COUNT * HEAD_SIZE) * jax.nn.sigmoid(gate_logit.astype(jnp.float32))
    return (normed_mixer_input.astype(jnp.bfloat16), matrix.reshape(tally_value, HEAD_COUNT, HEAD_SIZE * HEAD_SIZE))

def routed_sum(normed_ffn, routes, routing_weight, routed_gate_weight, routed_up_weight, routed_down_weight):
    tokens = normed_ffn.shape[0]
    limit = N_EP * CAP
    slots = jnp.arange(limit, dtype=jnp.int32)

    def add_expert(expert_id, total):
        match = routes == expert_id
        hit = jnp.any(match, axis=1).astype(jnp.int32)
        weight = lax.optimization_barrier(jnp.sum(jnp.where(match, routing_weight, 0.0), axis=1))
        rank = jnp.cumsum(hit) - hit
        select = (rank[None, :] == slots[:, None]) & (hit[None, :] == 1)
        rows = jnp.dot(select.astype(jnp.bfloat16), normed_ffn, preferred_element_type=jnp.float32).astype(jnp.bfloat16)
        output = expert_mlp(rows, routed_gate_weight[expert_id], routed_up_weight[expert_id], routed_down_weight[expert_id])
        spread = select.astype(jnp.float32).T * weight[:, None]
        return total + jnp.dot(spread, output.astype(jnp.float32), precision=lax.Precision.HIGHEST)
    return lax.fori_loop(0, EXPERTS, add_expert, jnp.zeros((tokens, normed_ffn.shape[1]), jnp.float32))

def reference(residual_input, attention_norm_gain, receptance_weight, key_weight, value_weight, decay_weight, correction_rate_weight, output_gate_weight, decay_offset, correction_rate_offset, self_term_weight, head_read_gain, previous_state, attention_output_weight, feedforward_norm_gain, routes, routing_weight, routed_gate_weight, routed_up_weight, routed_down_weight, common_gate_weight, common_up_weight, common_down_weight):
    normed = rms_norm(residual_input.astype(jnp.float32), attention_norm_gain)

    def apply_projection(weight):
        return jnp.dot(normed, weight, preferred_element_type=jnp.float32).astype(jnp.bfloat16)
    normed_mixer_input, next_state = attention_mixer(apply_projection(receptance_weight), apply_projection(key_weight), apply_projection(value_weight), apply_projection(decay_weight), apply_projection(correction_rate_weight), apply_projection(output_gate_weight), decay_offset, correction_rate_offset, self_term_weight, head_read_gain, previous_state)
    attended = jnp.dot(normed_mixer_input, attention_output_weight, preferred_element_type=jnp.float32).astype(jnp.bfloat16)
    middle = residual_input.astype(jnp.float32) + attended.astype(jnp.float32)
    normed_ffn = rms_norm(middle, feedforward_norm_gain)
    shared = expert_mlp(normed_ffn, common_gate_weight, common_up_weight, common_down_weight)
    routed = routed_sum(normed_ffn, routes, routing_weight, routed_gate_weight, routed_up_weight, routed_down_weight)
    hidden_out = (middle + shared.astype(jnp.float32) + routed).astype(jnp.bfloat16)
    return (hidden_out, next_state)
```

```python
import functools
import math

import jax
import jax.numpy as jnp
from jax import lax
from jax.experimental import pallas as pl
from jax.experimental.pallas import tpu as pltpu
from jax.sharding import PartitionSpec as P

HEAD_SIZE = 64
LANES = 128
ROLES = 6
CAP = 4
INNER = 4
MIDDLE = 2


F32 = jnp.float32
BF16 = jnp.bfloat16
VMEM = pltpu.MemorySpace.VMEM


def vmem_specs(count):
    return [pl.BlockSpec(memory_space=VMEM) for _ in range(count)]


def rms_rows(rows, gain):
    scale = lax.rsqrt(jnp.mean(rows * rows, axis=-1, keepdims=True) + 1e-06)
    return rows * scale * gain


def sigmoid(x):
    return 1.0 / (1.0 + jnp.exp(-x))


def prepare_kernel(residual_ref, gain_ref, *refs):
    weights, (normed_ref, packed_ref) = refs[:ROLES], refs[ROLES:]
    width = weights[0].shape[0]
    for role, ref in enumerate(weights):
        packed_ref[role * width : (role + 1) * width, :] = ref[...]
    rows = residual_ref[...].astype(F32)
    normed_ref[...] = rms_rows(rows, gain_ref[...].astype(F32)).astype(BF16)


def prepare(residual, gain, weights):
    depth, width = weights[0].shape
    return pl.pallas_call(
        prepare_kernel,
        out_shape=(
            jax.ShapeDtypeStruct(residual.shape, BF16),
            jax.ShapeDtypeStruct((ROLES * width, depth), BF16),
        ),
        in_specs=vmem_specs(2 + ROLES),
        out_specs=tuple(vmem_specs(2)),
        name="prepare",
    )(residual, gain.reshape(1, -1), *[w.T for w in weights])


def project_kernel(places, where_ref, *refs):
    chunks = refs[:places]
    packs = refs[places : places + INNER]
    out_ref, weight_ref = refs[places + INNER :]
    width = packs[0].shape[0] // ROLES
    lane_place, row_place = where_ref[0], where_ref[1]
    for near, ref in enumerate(packs):
        spot = jnp.bitwise_xor(lane_place, near)
        for role in range(ROLES):
            start = pl.multiple_of(role * INNER * width + spot * width, width)
            weight_ref[pl.ds(start, width), :] = ref[role * width : (role + 1) * width, :]
    rows = jnp.concatenate([ref[...].astype(F32) for ref in chunks], axis=0).astype(BF16)
    tally = chunks[0].shape[0]
    result = lax.dot_general(
        rows, weight_ref[...], (((1,), (1,)), ((), ())), preferred_element_type=F32
    )
    for near in range(places):
        out_ref[jnp.bitwise_xor(row_place, near)] = result[
            near * tally : (near + 1) * tally
        ].astype(BF16)


def project(where, chunks, packs):
    places = len(chunks)
    tally, depth = chunks[0].shape
    rows = packs[0].shape[0] * INNER
    return pl.pallas_call(
        functools.partial(project_kernel, places),
        out_shape=jax.ShapeDtypeStruct((places, tally, rows), BF16),
        in_specs=[pl.BlockSpec(memory_space=pltpu.MemorySpace.SMEM)]
        + vmem_specs(places + INNER),
        out_specs=vmem_specs(1)[0],
        scratch_shapes=[pltpu.VMEM((rows, depth), BF16)],
        cost_estimate=pl.CostEstimate(
            flops=2 * places * tally * rows * depth,
            bytes_accessed=2 * rows * depth,
            transcendentals=0,
        ),
        name="project",
    )(where, *chunks, *packs)


def route_kernel(routes_ref, turned_ref, weight_ref, select_ref, blend_ref):
    tally, top = routes_ref.shape
    slots = select_ref.shape[0]
    lane = lax.broadcasted_iota(jnp.int32, (tally, slots), 1)
    hit = jnp.zeros((tally, slots), F32)
    weight = jnp.zeros((tally, slots), F32)
    for j in range(top):
        match = routes_ref[:, j : j + 1] == lax.div(lane, CAP)
        hit = jnp.where(match, 1.0, hit)
        weight = weight + jnp.where(match, weight_ref[:, j : j + 1], 0.0)
    row = lax.broadcasted_iota(jnp.int32, (tally, tally), 0)
    column = lax.broadcasted_iota(jnp.int32, (tally, tally), 1)
    rank = jnp.dot((column < row).astype(F32), hit, preferred_element_type=F32)
    chosen = (hit > 0.5) & (rank.astype(jnp.int32) == lax.rem(lane, CAP))
    blend_ref[...] = jnp.where(chosen, weight, 0.0)
    slot = lax.broadcasted_iota(jnp.int32, (slots, tally), 0)
    hit = jnp.zeros((slots, tally), F32)
    for j in range(top):
        hit = jnp.where(turned_ref[j : j + 1, :] == lax.div(slot, CAP), 1.0, hit)
    rank = jnp.dot(hit, (row < column).astype(F32), preferred_element_type=F32)
    chosen = (hit > 0.5) & (rank.astype(jnp.int32) == lax.rem(slot, CAP))
    select_ref[...] = jnp.where(chosen, 1.0, 0.0).astype(BF16)


def route(routes, weight, experts):
    tally = routes.shape[0]
    slots = experts * CAP
    return pl.pallas_call(
        route_kernel,
        out_shape=(
            jax.ShapeDtypeStruct((slots, tally), BF16),
            jax.ShapeDtypeStruct((tally, slots), F32),
        ),
        in_specs=vmem_specs(3),
        out_specs=tuple(vmem_specs(2)),
        name="route",
    )(routes, routes.T, weight)


def segment_sum(values):
    row = lax.broadcasted_iota(jnp.int32, (LANES, LANES), 0)
    column = lax.broadcasted_iota(jnp.int32, (LANES, LANES), 1)
    ones = (lax.div(row, HEAD_SIZE) == lax.div(column, HEAD_SIZE)).astype(F32)
    return jnp.dot(values, ones, preferred_element_type=F32, precision=lax.Precision.HIGHEST)


def fold(left, right, length, lane):
    half = length // 2
    low = jnp.bitwise_and(lane, half) == 0
    straight = jnp.where(low, left, right)
    turned = jnp.where(
        low, pltpu.roll(left, LANES - half, 1), pltpu.roll(right, half, 1)
    )
    return straight + turned


def reverse_bits(lane):
    bits = int(math.log2(LANES))
    result = jnp.zeros_like(lane)
    for i in range(bits):
        bit = jnp.bitwise_and(lax.shift_right_logical(lane, i), 1)
        result = result + bit * (1 << (bits - 1 - i))
    return result


def join(first, first_half, second, second_half):
    lane = lax.broadcasted_iota(jnp.int32, first.shape, 1)
    low = first if first_half == 0 else pltpu.roll(first, HEAD_SIZE, 1)
    high = second if second_half == 1 else pltpu.roll(second, HEAD_SIZE, 1)
    return jnp.where(lane < HEAD_SIZE, low, high)


def twice(parts, head):
    return join(parts[head // 2], head % 2, parts[head // 2], head % 2)


def spread_heads(parts):
    count = len(parts)
    return [
        join(parts[j // 2], j % 2, parts[count // 2 + j // 2], j % 2) for j in range(count)
    ]


def pair_heads(parts):
    count = len(parts)
    return [
        join(
            parts[2 * b % count],
            2 * b // count,
            parts[(2 * b + 1) % count],
            (2 * b + 1) // count,
        )
        for b in range(count)
    ]


def attend_kernel(
    mixed_cols_ref,
    vector_ref,
    state_ref,
    residual_ref,
    gain_ref,
    select_ref,
    output_hbm,
    send_ref,
    ffn_ref,
    middle_ref,
    decay_ref,
    scaled_ref,
    update_ref,
    unit_ref,
    faded_ref,
    norm_ref,
    value_ref,
    gate_ref,
    own_ref,
    dot_ref,
    recall_ref,
    read_ref,
    square_ref,
    cross_ref,
    self_ref,
    mixed_ref,
    weight_ref,
    weight_sem,
):
    step = pl.program_id(0)
    blocks, tally, _ = mixed_cols_ref.shape
    copy = pltpu.make_async_copy(output_hbm, weight_ref, weight_sem)

    @pl.when(step == 0)
    def _():
        copy.start()
        for b in range(blocks):
            rows = pl.ds(b * tally, tally)

            def part(role):
                return mixed_cols_ref[b, :, role * LANES : (role + 1) * LANES].astype(F32)

            def vector(which):
                return vector_ref[which, b : b + 1, :]

            receptance, key, value = part(0), part(1), part(2)
            decay = jnp.exp(-math.exp(-0.5) * sigmoid(vector(0) + part(3)))
            rate = sigmoid(vector(1) + part(4))
            scaled = key * rate
            cross = receptance * scaled
            square_ref[rows, :] = key * key
            cross_ref[rows, :] = cross
            self_ref[rows, :] = cross * vector(2)
            value_ref[rows, :] = value
            gate_ref[rows, :] = sigmoid(part(5))
            for h in range(2):
                wide = pl.ds((2 * b + h) * tally, tally)
                decay_ref[wide, :] = join(decay, h, decay, h)
                scaled_ref[wide, :] = join(scaled, h, scaled, h)
                faded = decay * receptance
                faded_ref[wide, :] = join(faded, h, faded, h)
        norm = lax.rsqrt(1.0 + segment_sum(square_ref[...]))
        norm_ref[...] = norm
        for b in range(blocks):
            rows = slice(b * tally, (b + 1) * tally)
            key = mixed_cols_ref[b, :, LANES : 2 * LANES].astype(F32)
            unit = key * norm[rows]
            for h in range(2):
                unit_ref[pl.ds((2 * b + h) * tally, tally), :] = join(unit, h, unit, h)
        dot_ref[...] = segment_sum(cross_ref[...])
        own_ref[...] = segment_sum(self_ref[...])

    per_step = state_ref.shape[0]
    tiles = state_ref.shape[2] // LANES
    lane = lax.broadcasted_iota(jnp.int32, (blocks, LANES), 1)
    order = reverse_bits(lane)

    def token(i, carry):
        at = pl.ds(step * per_step + i, blocks, stride=tally)
        sources = [
            pl.ds(side * blocks * tally + step * per_step + i, blocks, stride=tally)
            for side in range(2)
        ]
        units = [unit_ref[source, :] for source in sources]
        fades = [faded_ref[source, :] for source in sources]

        def reduce(side, first, count):
            if count == 1:
                tile = state_ref[
                    i,
                    side * blocks : (side + 1) * blocks,
                    first * LANES : (first + 1) * LANES,
                ]
                return tile * units[side], tile * fades[side]
            half = count // 2
            left = reduce(side, first, half)
            right = reduce(side, first + half, half)
            length = 2 * HEAD_SIZE // count
            return tuple(fold(a, b, length, lane) for a, b in zip(left, right))

        low, high = reduce(0, 0, tiles), reduce(1, 0, tiles)
        recall, read = (fold(a, b, 2, lane) for a, b in zip(low, high))
        recall_ref[at, :] = jnp.take_along_axis(recall, order, axis=1)
        read_ref[at, :] = jnp.take_along_axis(read, order, axis=1)
        return carry

    lax.fori_loop(0, per_step, token, 0)

    @pl.when(step == pl.num_programs(0) - 1)
    def _():
        def blockwise(array):
            return [array[b * tally : (b + 1) * tally] for b in range(blocks)]

        recall = jnp.concatenate(pair_heads(blockwise(recall_ref[...])), axis=0)
        read = jnp.concatenate(pair_heads(blockwise(read_ref[...])), axis=0)
        update = value_ref[...] - recall * norm_ref[...]
        for j, part in enumerate(spread_heads(blockwise(update))):
            update_ref[j * tally : (j + 1) * tally, :] = part
        read = read + update * dot_ref[...]
        centered = read - segment_sum(read) * (1.0 / HEAD_SIZE)
        variance = segment_sum(centered * centered) * (1.0 / HEAD_SIZE)
        normal = centered * lax.rsqrt(variance + 0.00064)
        own = own_ref[...] * value_ref[...]
        gate = gate_ref[...]
        for b in range(blocks):
            rows = slice(b * tally, (b + 1) * tally)
            mixed_ref[:, b * LANES : (b + 1) * LANES] = (
                (normal[rows] * vector_ref[3, b : b + 1, :] + own[rows]) * gate[rows]
            ).astype(BF16)
        copy.wait()
        attended = jnp.dot(mixed_ref[...], weight_ref[...], preferred_element_type=F32)
        middle = residual_ref[...].astype(F32) + attended.astype(BF16).astype(F32)
        middle_ref[...] = middle
        ffn = rms_rows(middle, gain_ref[...].astype(F32)).astype(BF16)
        ffn_ref[...] = ffn
        send_ref[...] = jnp.dot(
            select_ref[...], ffn, preferred_element_type=F32
        ).astype(BF16)


def state_steps(tally):
    return max(k for k in (1, 2, 3, 4) if tally % k == 0)


def attend(columns, vectors, state, residual, gain, select, output_weight):
    blocks, tally, _ = columns.shape
    depth = residual.shape[1]
    slots = select.shape[0]
    steps = state_steps(tally)
    rows = blocks * tally

    def whole(shape):
        return pl.BlockSpec(shape, lambda i: (0,) * len(shape))

    flat = jax.ShapeDtypeStruct((rows, LANES), F32)
    wide = jax.ShapeDtypeStruct((2 * rows, LANES), F32)
    return pl.pallas_call(
        attend_kernel,
        grid=(steps,),
        out_shape=(
            jax.ShapeDtypeStruct((slots, depth), BF16),
            jax.ShapeDtypeStruct((tally, depth), BF16),
            jax.ShapeDtypeStruct((tally, depth), F32),
            wide,
            wide,
            flat,
        ),
        in_specs=[
            whole(columns.shape),
            whole(vectors.shape),
            pl.BlockSpec((tally // steps,) + state.shape[1:], lambda i: (i, 0, 0)),
            whole(residual.shape),
            whole((1, depth)),
            whole(select.shape),
            pl.BlockSpec(memory_space=pl.ANY),
        ],
        out_specs=(
            whole((slots, depth)),
            whole((tally, depth)),
            whole((tally, depth)),
            whole((2 * rows, LANES)),
            whole((2 * rows, LANES)),
            whole((rows, LANES)),
        ),
        scratch_shapes=[pltpu.VMEM((2 * rows, LANES), F32) for _ in range(2)]
        + [pltpu.VMEM((rows, LANES), F32) for _ in range(10)]
        + [
            pltpu.VMEM((tally, blocks * LANES), BF16),
            pltpu.VMEM(output_weight.shape, BF16),
            pltpu.SemaphoreType.DMA,
        ],
        cost_estimate=pl.CostEstimate(
            flops=8 * state.size, bytes_accessed=4 * state.size, transcendentals=0
        ),
        name="attend",
    )(columns, vectors, state, residual, gain.reshape(1, -1), select, output_weight)


def update_kernel(state_ref, decay_ref, scaled_ref, update_ref, out_ref):
    step = pl.program_id(0)
    per_step = state_ref.shape[0]
    blocks = state_ref.shape[1] // 2
    tally = update_ref.shape[0] // blocks
    tiles = state_ref.shape[2] // LANES
    lane = lax.broadcasted_iota(jnp.int32, (blocks, LANES), 1)
    half = lax.div(lane, HEAD_SIZE)

    def token(i, carry):
        spot = step * per_step + i
        update = update_ref[pl.ds(spot, blocks, stride=tally), :]
        for side in range(2):
            source = pl.ds(side * blocks * tally + spot, blocks, stride=tally)
            decay, scaled = decay_ref[source, :], scaled_ref[source, :]
            heads = slice(side * blocks, (side + 1) * blocks)
            for tile in range(tiles):
                lanes = slice(tile * LANES, (tile + 1) * LANES)
                where = half + (side * HEAD_SIZE + 2 * tile)
                spread = jnp.take_along_axis(update, where, axis=1)
                out_ref[i, heads, lanes] = state_ref[i, heads, lanes] * decay + spread * scaled
        return carry

    lax.fori_loop(0, per_step, token, 0)


def update_state(state, decay, scaled, update):
    tally = state.shape[0]
    steps = state_steps(tally)
    wide = pl.BlockSpec(decay.shape, lambda i: (0, 0))
    flat = pl.BlockSpec(update.shape, lambda i: (0, 0))
    block = pl.BlockSpec((tally // steps,) + state.shape[1:], lambda i: (i, 0, 0))
    return pl.pallas_call(
        update_kernel,
        grid=(steps,),
        out_shape=jax.ShapeDtypeStruct(state.shape, F32),
        in_specs=[block, wide, wide, flat],
        out_specs=block,
        cost_estimate=pl.CostEstimate(
            flops=3 * state.size, bytes_accessed=8 * state.size, transcendentals=0
        ),
        name="update_state",
    )(state, decay, scaled, update)


def expert_mlp(rows, gate_w, up_w, down_w):
    gate = jnp.dot(rows, gate_w, preferred_element_type=F32)
    upward = jnp.dot(rows, up_w, preferred_element_type=F32)
    hidden = (jax.nn.silu(gate) * upward).astype(BF16)
    return jnp.dot(hidden, down_w, preferred_element_type=F32).astype(BF16)


def per_device(
    residual_input,
    attention_norm_gain,
    receptance_weight,
    key_weight,
    value_weight,
    decay_weight,
    correction_rate_weight,
    output_gate_weight,
    decay_offset,
    correction_rate_offset,
    self_term_weight,
    head_read_gain,
    previous_state,
    attention_output_weight,
    feedforward_norm_gain,
    routes,
    routing_weight,
    routed_gate_weight,
    routed_up_weight,
    routed_down_weight,
    common_gate_weight,
    common_up_weight,
    common_down_weight,
):
    ep_size = lax.axis_size("ep")
    device = lax.axis_index("ep")
    tally = residual_input.shape[0]
    places = ep_size // INNER
    outer = places // MIDDLE

    def flip(array, mask):
        return lax.ppermute(array, "ep", [(s, s ^ mask) for s in range(ep_size)])

    normed, pack = prepare(
        residual_input,
        attention_norm_gain,
        (
            receptance_weight,
            key_weight,
            value_weight,
            decay_weight,
            correction_rate_weight,
            output_gate_weight,
        ),
    )
    side = flip(pack, 2)
    packs = [pack, flip(pack, 1), side, flip(side, 1)]
    chunks = [None] * places
    for k in range(outer):
        chunk = normed if k == 0 else flip(normed, INNER * MIDDLE * k)
        chunks[MIDDLE * k] = chunk
        chunks[MIDDLE * k + 1] = flip(chunk, INNER)
    where = jnp.stack([lax.rem(device, INNER), lax.div(device, INNER)]).astype(jnp.int32)
    projected = project(where, chunks, packs)
    groups = [[p * INNER + q for p in range(places)] for q in range(INNER)]
    columns = lax.all_to_all(
        projected, "ep", split_axis=0, concat_axis=0, tiled=True, axis_index_groups=groups
    )

    expert_count = routed_gate_weight.shape[0] * ep_size
    own_routes = lax.dynamic_slice_in_dim(routes, device * tally, tally, 0)
    own_weight = lax.dynamic_slice_in_dim(routing_weight, device * tally, tally, 0)
    select, blend = route(own_routes, own_weight, expert_count)

    vectors = jnp.stack(
        [decay_offset, correction_rate_offset, self_term_weight, head_read_gain]
    ).reshape(4, places, LANES)
    send, normed_ffn, middle, decay, scaled, update = attend(
        columns,
        vectors,
        previous_state,
        residual_input,
        feedforward_norm_gain,
        select,
        attention_output_weight,
    )
    depth = residual_input.shape[1]
    rows = lax.all_to_all(
        send.reshape(ep_size, CAP, depth), "ep", split_axis=0, concat_axis=0, tiled=True
    )
    next_state = update_state(previous_state, decay, scaled, update)
    shared = expert_mlp(normed_ffn, common_gate_weight, common_up_weight, common_down_weight)
    output = expert_mlp(
        rows.reshape(ep_size * CAP, depth),
        routed_gate_weight[0],
        routed_up_weight[0],
        routed_down_weight[0],
    )
    returned = lax.all_to_all(
        output.reshape(ep_size, CAP, depth), "ep", split_axis=0, concat_axis=0, tiled=True
    )
    routed = jnp.dot(
        blend,
        returned.reshape(ep_size * CAP, depth).astype(F32),
        precision=lax.Precision.HIGHEST,
    )
    hidden_out = (middle + shared.astype(F32) + routed).astype(BF16)
    return (hidden_out, next_state)


def solution(mesh):
    return jax.shard_map(
        per_device,
        mesh=mesh,
        in_specs=(
            P(("grp", "ep"), None),
            P(),
            P(None, "ep"),
            P(None, "ep"),
            P(None, "ep"),
            P(None, "ep"),
            P(None, "ep"),
            P(None, "ep"),
            P(),
            P(),
            P(),
            P(),
            P(("grp", "ep"), None, None),
            P(),
            P(),
            P("grp", None),
            P("grp", None),
            P("ep", None, None),
            P("ep", None, None),
            P("ep", None, None),
            P(),
            P(),
            P(),
        ),
        out_specs=(P(("grp", "ep"), None), P(("grp", "ep"), None, None)),
        check_vma=False,
    )
```

```python
import functools
import math

import jax
import jax.numpy as jnp
from jax import lax
from jax.experimental import pallas as pl
from jax.experimental.pallas import tpu as pltpu
from jax.sharding import PartitionSpec as P

HEAD_SIZE = 64
LANES = 128
ROLES = 6
CAP = 4
INNER = 4
MIDDLE = 2


F32 = jnp.float32
BF16 = jnp.bfloat16
VMEM = pltpu.MemorySpace.VMEM
HBM = pltpu.MemorySpace.HBM


def vmem_specs(count):
    return [pl.BlockSpec(memory_space=VMEM) for _ in range(count)]


def hbm_specs(count):
    return [pl.BlockSpec(memory_space=HBM) for _ in range(count)]


def limit(mebibytes):
    return pltpu.CompilerParams(vmem_limit_bytes=mebibytes << 20)


def scaled_rows(rows, gain):
    width = gain.shape[1]
    scale = lax.rsqrt(jnp.mean(rows * rows, axis=-1, keepdims=True) + 1e-06)
    parts = [
        rows[:, j * width : (j + 1) * width] * scale * gain[j : j + 1].astype(F32)
        for j in range(gain.shape[0])
    ]
    return jnp.concatenate(parts, axis=1).astype(BF16)


def sigmoid(x):
    return 1.0 / (1.0 + jnp.exp(-x))


def prepare_kernel(residual_hbm, gain_hbm, *refs):
    weights = refs[:ROLES]
    normed_ref, packed_ref, residual_ref, gain_ref, sems = refs[ROLES:]
    width = weights[0].shape[0]
    copies = [
        pltpu.make_async_copy(residual_hbm, residual_ref, sems.at[0]),
        pltpu.make_async_copy(gain_hbm, gain_ref, sems.at[1]),
    ] + [
        pltpu.make_async_copy(
            ref, packed_ref.at[role * width : (role + 1) * width, :], sems.at[2 + role]
        )
        for role, ref in enumerate(weights)
    ]
    for copy in copies:
        copy.start()
    copies[0].wait()
    copies[1].wait()
    normed_ref[...] = scaled_rows(residual_ref[...].astype(F32), gain_ref[...])
    for copy in copies[2:]:
        copy.wait()


def prepare(residual, gain, weights):
    depth, width = weights[0].shape
    gain = gain.reshape(-1, LANES)
    return pl.pallas_call(
        prepare_kernel,
        out_shape=(
            jax.ShapeDtypeStruct(residual.shape, BF16),
            jax.ShapeDtypeStruct((ROLES * width, depth), BF16),
        ),
        in_specs=hbm_specs(2 + ROLES),
        out_specs=tuple(vmem_specs(2)),
        scratch_shapes=[
            pltpu.VMEM(residual.shape, BF16),
            pltpu.VMEM(gain.shape, BF16),
            pltpu.SemaphoreType.DMA((2 + ROLES,)),
        ],
        compiler_params=limit(60),
        name="prepare",
    )(residual, gain, *[w.T for w in weights])


def project_kernel(places, where_ref, *refs):
    chunks = refs[:places]
    packs = refs[places : places + INNER]
    out_ref, rows_ref, weight_ref, row_sems, weight_sems = refs[places + INNER :]
    width = packs[0].shape[0] // ROLES
    tally = out_ref.shape[1]
    lane_place, row_place = where_ref[0], where_ref[1]
    row_copies = [
        pltpu.make_async_copy(ref, rows_ref.at[near], row_sems.at[near])
        for near, ref in enumerate(chunks)
    ]
    weight_copies = []
    for role in range(ROLES):
        for near, ref in enumerate(packs):
            spot = jnp.bitwise_xor(lane_place, near)
            start = pl.multiple_of((role * INNER + spot) * width, width)
            weight_copies.append(
                pltpu.make_async_copy(
                    ref.at[role * width : (role + 1) * width, :],
                    weight_ref.at[pl.ds(start, width), :],
                    weight_sems.at[role, near],
                )
            )
    for copy in row_copies + weight_copies:
        copy.start()
    for copy in row_copies:
        copy.wait()
    rows = jnp.concatenate([rows_ref[k].astype(F32) for k in range(places)], axis=0).astype(BF16)
    for copy in weight_copies:
        copy.wait()
    result = lax.dot_general(
        rows, weight_ref[...], (((1,), (1,)), ((), ())), preferred_element_type=F32
    )
    for near in range(places):
        out_ref[jnp.bitwise_xor(row_place, near)] = result[
            near * tally : (near + 1) * tally
        ].astype(BF16)


def project(where, chunks, packs):
    places = len(chunks)
    tally, depth = chunks[0].shape
    rows = packs[0].shape[0] * INNER
    return pl.pallas_call(
        functools.partial(project_kernel, places),
        out_shape=jax.ShapeDtypeStruct((places, tally, rows), BF16),
        in_specs=[pl.BlockSpec(memory_space=pltpu.MemorySpace.SMEM)]
        + hbm_specs(places + INNER),
        out_specs=vmem_specs(1)[0],
        scratch_shapes=[
            pltpu.VMEM((places, tally, depth), BF16),
            pltpu.VMEM((rows, depth), BF16),
            pltpu.SemaphoreType.DMA((places,)),
            pltpu.SemaphoreType.DMA((ROLES, INNER)),
        ],
        cost_estimate=pl.CostEstimate(
            flops=2 * places * tally * rows * depth,
            bytes_accessed=2 * rows * depth,
            transcendentals=0,
        ),
        compiler_params=limit(60),
        name="project",
    )(where, *chunks, *packs)


def linger_kernel(in_ref, out_ref):
    out_ref[...] = in_ref[...]


def linger(array, nanoseconds):
    return pl.pallas_call(
        linger_kernel,
        out_shape=jax.ShapeDtypeStruct(array.shape, array.dtype),
        in_specs=vmem_specs(1),
        out_specs=vmem_specs(1)[0],
        cost_estimate=pl.CostEstimate(
            flops=nanoseconds * 500_000, bytes_accessed=0, transcendentals=0
        ),
        compiler_params=limit(1),
        name="linger",
    )(array)


def route_kernel(routes_ref, turned_ref, weight_ref, select_ref, blend_ref):
    tally, top = routes_ref.shape
    halves, slots, _ = select_ref.shape
    chunk = halves * CAP
    lane = lax.broadcasted_iota(jnp.int32, (tally, slots), 1)
    hit = jnp.zeros((tally, slots), F32)
    weight = jnp.zeros((tally, slots), F32)
    for j in range(top):
        match = routes_ref[:, j : j + 1] == lax.div(lane, chunk)
        hit = jnp.where(match, 1.0, hit)
        weight = weight + jnp.where(match, weight_ref[:, j : j + 1], 0.0)
    row = lax.broadcasted_iota(jnp.int32, (tally, tally), 0)
    column = lax.broadcasted_iota(jnp.int32, (tally, tally), 1)
    rank = jnp.dot((column < row).astype(F32), hit, preferred_element_type=F32)
    chosen = (hit > 0.5) & (rank.astype(jnp.int32) == lax.rem(lane, CAP))
    for half in range(halves):
        here = chosen & (lax.rem(lax.div(lane, CAP), halves) == half)
        blend = jnp.where(here, weight, 0.0)
        coarse = blend.astype(BF16)
        blend_ref[half, 0] = coarse
        blend_ref[half, 1] = (blend - coarse.astype(F32)).astype(BF16)
    slot = lax.broadcasted_iota(jnp.int32, (slots, tally), 0)
    hit = jnp.zeros((slots, tally), F32)
    for j in range(top):
        hit = jnp.where(turned_ref[j : j + 1, :] == lax.div(slot, chunk), 1.0, hit)
    rank = jnp.dot(hit, (row < column).astype(F32), preferred_element_type=F32)
    chosen = (hit > 0.5) & (rank.astype(jnp.int32) == lax.rem(slot, CAP))
    for half in range(halves):
        here = chosen & (lax.rem(lax.div(slot, CAP), halves) == half)
        select_ref[half] = jnp.where(here, 1.0, 0.0).astype(BF16)


def route(routes, weight, experts, halves):
    tally = routes.shape[0]
    slots = experts * CAP * halves
    return pl.pallas_call(
        route_kernel,
        out_shape=(
            jax.ShapeDtypeStruct((halves, slots, tally), BF16),
            jax.ShapeDtypeStruct((halves, 2, tally, slots), BF16),
        ),
        in_specs=vmem_specs(3),
        out_specs=tuple(vmem_specs(2)),
        compiler_params=limit(4),
        name="route",
    )(routes, routes.T, weight)


def segment_sum(values):
    row = lax.broadcasted_iota(jnp.int32, (LANES, LANES), 0)
    column = lax.broadcasted_iota(jnp.int32, (LANES, LANES), 1)
    ones = (lax.div(row, HEAD_SIZE) == lax.div(column, HEAD_SIZE)).astype(F32)
    return jnp.dot(values, ones, preferred_element_type=F32, precision=lax.Precision.HIGHEST)


def join(first, first_half, second, second_half):
    lane = lax.broadcasted_iota(jnp.int32, first.shape, 1)
    low = first if first_half == 0 else pltpu.roll(first, HEAD_SIZE, 1)
    high = second if second_half == 1 else pltpu.roll(second, HEAD_SIZE, 1)
    return jnp.where(lane < HEAD_SIZE, low, high)


def twice(parts, head):
    return join(parts[head // 2], head % 2, parts[head // 2], head % 2)


def spread_heads(parts):
    count = len(parts)
    return [
        join(parts[j // 2], j % 2, parts[count // 2 + j // 2], j % 2) for j in range(count)
    ]


def pair_heads(parts):
    count = len(parts)
    return [
        join(
            parts[2 * b % count],
            2 * b // count,
            parts[(2 * b + 1) % count],
            (2 * b + 1) // count,
        )
        for b in range(count)
    ]


def attend_kernel(
    mixed_cols_ref,
    vector_ref,
    state_ref,
    residual_ref,
    gain_ref,
    select_ref,
    weight_ref,
    send_ref,
    ffn_ref,
    middle_ref,
    decay_ref,
    scaled_ref,
    update_ref,
    unit_ref,
    faded_ref,
    norm_ref,
    value_ref,
    gate_ref,
    own_ref,
    dot_ref,
    recall_ref,
    read_ref,
    square_ref,
    cross_ref,
    self_ref,
    product_ref,
    ones_ref,
    mixed_ref,
):
    blocks, tally, _ = mixed_cols_ref.shape
    _, heads, width = state_ref.shape
    tiles = width // LANES
    per_step = product_ref.shape[0] // (2 * heads)
    steps = tally // per_step

    row = lax.broadcasted_iota(jnp.int32, ones_ref.shape, 0)
    column = lax.broadcasted_iota(jnp.int32, ones_ref.shape, 1)
    same = lax.div(row, HEAD_SIZE) == lax.rem(column, HEAD_SIZE)
    ones_ref[...] = same.astype(F32).astype(BF16)
    for b in range(blocks):
        rows = pl.ds(b * tally, tally)

        def part(role):
            return mixed_cols_ref[b, :, role * LANES : (role + 1) * LANES].astype(F32)

        def vector(which):
            return vector_ref[which, b : b + 1, :]

        receptance, key, value = part(0), part(1), part(2)
        decay = jnp.exp(-math.exp(-0.5) * sigmoid(vector(0) + part(3)))
        rate = sigmoid(vector(1) + part(4))
        scaled = key * rate
        cross = receptance * scaled
        faded = decay * receptance
        square_ref[rows, :] = key * key
        cross_ref[rows, :] = cross
        self_ref[rows, :] = cross * vector(2)
        value_ref[rows, :] = value
        gate_ref[rows, :] = sigmoid(part(5))
        for h in range(2):
            wide = pl.ds((2 * b + h) * tally, tally)
            decay_ref[wide, :] = join(decay, h, decay, h)
            scaled_ref[wide, :] = join(scaled, h, scaled, h)
            faded_ref[wide, :] = join(faded, h, faded, h)
    norm = lax.rsqrt(1.0 + segment_sum(square_ref[...]))
    norm_ref[...] = norm
    for b in range(blocks):
        rows = slice(b * tally, (b + 1) * tally)
        key = mixed_cols_ref[b, :, LANES : 2 * LANES].astype(F32)
        unit = key * norm[rows]
        for h in range(2):
            unit_ref[pl.ds((2 * b + h) * tally, tally), :] = join(unit, h, unit, h)
    dot_ref[...] = segment_sum(cross_ref[...])
    own_ref[...] = segment_sum(self_ref[...])

    first = lax.broadcasted_iota(jnp.int32, (blocks, LANES), 1) < HEAD_SIZE

    def step_tokens(step, carry):
        def token(i, carry):
            spot = step * per_step + i
            source = pl.ds(spot, heads, stride=tally)
            unit, faded = unit_ref[source, :], faded_ref[source, :]
            row = pl.multiple_of(2 * heads * i, 2 * heads)
            for tile in range(tiles):
                lanes = slice(tile * LANES, (tile + 1) * LANES)
                state = state_ref[spot, :, lanes]
                product_ref[pl.ds(row, heads), lanes] = (state * unit).astype(BF16)
                product_ref[pl.ds(row + heads, heads), lanes] = (state * faded).astype(BF16)
            return carry

        lax.fori_loop(0, per_step, token, 0)
        sums = jnp.dot(product_ref[...], ones_ref[...], preferred_element_type=F32)
        for i in range(per_step):
            at = pl.ds(step * per_step + i, blocks, stride=tally)
            for which, ref in enumerate((recall_ref, read_ref)):
                row = (2 * i + which) * heads
                ref[at, :] = jnp.where(
                    first, sums[row : row + blocks], sums[row + blocks : row + heads]
                )
        return carry

    lax.fori_loop(0, steps, step_tokens, 0)

    def blockwise(array):
        return [array[b * tally : (b + 1) * tally] for b in range(blocks)]

    recall = jnp.concatenate(pair_heads(blockwise(recall_ref[...])), axis=0)
    read = jnp.concatenate(pair_heads(blockwise(read_ref[...])), axis=0)
    update = value_ref[...] - recall * norm_ref[...]
    for j, part in enumerate(spread_heads(blockwise(update))):
        update_ref[j * tally : (j + 1) * tally, :] = part
    read = read + update * dot_ref[...]
    centered = read - segment_sum(read) * (1.0 / HEAD_SIZE)
    variance = segment_sum(centered * centered) * (1.0 / HEAD_SIZE)
    normal = centered * lax.rsqrt(variance + 0.00064)
    own = own_ref[...] * value_ref[...]
    gate = gate_ref[...]
    for b in range(blocks):
        rows = slice(b * tally, (b + 1) * tally)
        mixed_ref[:, b * LANES : (b + 1) * LANES] = (
            (normal[rows] * vector_ref[3, b : b + 1, :] + own[rows]) * gate[rows]
        ).astype(BF16)
    attended = jnp.dot(mixed_ref[...], weight_ref[...], preferred_element_type=F32)
    middle = residual_ref[...].astype(F32) + attended.astype(BF16).astype(F32)
    middle_ref[...] = middle
    ffn = scaled_rows(middle, gain_ref[...])
    ffn_ref[...] = ffn
    halves = select_ref.shape[0]
    wide = ffn.shape[1] // halves
    send_ref[...] = sum(
        jnp.dot(
            select_ref[half],
            ffn[:, half * wide : (half + 1) * wide],
            preferred_element_type=F32,
        )
        for half in range(halves)
    ).astype(BF16)


def attend(columns, vectors, state, residual, gain, select, output_weight):
    blocks, tally, _ = columns.shape
    depth = residual.shape[1]
    halves, slots, _ = select.shape
    rows = blocks * tally
    per_step = tally // 2 if tally % 2 == 0 else tally
    flat = jax.ShapeDtypeStruct((rows, LANES), F32)
    wide = jax.ShapeDtypeStruct((2 * rows, LANES), F32)
    return pl.pallas_call(
        attend_kernel,
        out_shape=(
            jax.ShapeDtypeStruct((slots, depth // halves), BF16),
            jax.ShapeDtypeStruct((tally, depth), BF16),
            jax.ShapeDtypeStruct((tally, depth), F32),
            wide,
            wide,
            flat,
        ),
        in_specs=vmem_specs(7),
        out_specs=tuple(vmem_specs(6)),
        scratch_shapes=[pltpu.VMEM((2 * rows, LANES), F32) for _ in range(2)]
        + [pltpu.VMEM((rows, LANES), F32) for _ in range(10)]
        + [
            pltpu.VMEM((2 * per_step * state.shape[1], state.shape[2]), BF16),
            pltpu.VMEM((state.shape[2], LANES), BF16),
            pltpu.VMEM((tally, blocks * LANES), BF16),
        ],
        cost_estimate=pl.CostEstimate(
            flops=8 * state.size, bytes_accessed=4 * state.size, transcendentals=0
        ),
        compiler_params=limit(28),
        name="attend",
    )(columns, vectors, state, residual, gain.reshape(-1, LANES), select, output_weight)


def state_steps(tally):
    return max(k for k in (1, 2, 3, 4) if tally % k == 0)


def update_kernel(state_ref, decay_ref, scaled_ref, update_ref, out_ref):
    step = pl.program_id(0)
    per_step = state_ref.shape[0]
    blocks = state_ref.shape[1] // 2
    tally = update_ref.shape[0] // blocks
    tiles = state_ref.shape[2] // LANES
    lane = lax.broadcasted_iota(jnp.int32, (blocks, LANES), 1)
    half = lax.div(lane, HEAD_SIZE)

    def token(i, carry):
        spot = step * per_step + i
        update = update_ref[pl.ds(spot, blocks, stride=tally), :]
        for side in range(2):
            source = pl.ds(side * blocks * tally + spot, blocks, stride=tally)
            decay, scaled = decay_ref[source, :], scaled_ref[source, :]
            heads = slice(side * blocks, (side + 1) * blocks)
            for tile in range(tiles):
                lanes = slice(tile * LANES, (tile + 1) * LANES)
                where = half + (side * HEAD_SIZE + 2 * tile)
                spread = jnp.take_along_axis(update, where, axis=1)
                out_ref[i, heads, lanes] = state_ref[i, heads, lanes] * decay + spread * scaled
        return carry

    lax.fori_loop(0, per_step, token, 0)


def update_state(state, decay, scaled, update):
    tally = state.shape[0]
    steps = state_steps(tally)
    wide = pl.BlockSpec(decay.shape, lambda i: (0, 0))
    flat = pl.BlockSpec(update.shape, lambda i: (0, 0))
    block = pl.BlockSpec((tally // steps,) + state.shape[1:], lambda i: (i, 0, 0))
    return pl.pallas_call(
        update_kernel,
        grid=(steps,),
        out_shape=jax.ShapeDtypeStruct(state.shape, F32),
        in_specs=[block, wide, wide, flat],
        out_specs=block,
        cost_estimate=pl.CostEstimate(
            flops=3 * state.size, bytes_accessed=8 * state.size, transcendentals=0
        ),
        compiler_params=limit(60),
        name="update_state",
    )(state, decay, scaled, update)


def expert_mlp(rows, gate_w, up_w, down_w):
    gate = jnp.dot(rows, gate_w, preferred_element_type=F32)
    upward = jnp.dot(rows, up_w, preferred_element_type=F32)
    hidden = (jax.nn.silu(gate) * upward).astype(BF16)
    return jnp.dot(hidden, down_w, preferred_element_type=F32).astype(BF16)


def expert_kernel(rows_ref, gate_ref, up_ref, down_ref, out_ref):
    wide = rows_ref.shape[1]
    halves = gate_ref.shape[0] // wide
    rows = rows_ref[...]
    spot = lax.rem(
        lax.div(lax.broadcasted_iota(jnp.int32, (rows.shape[0], 1), 0), CAP), halves
    )
    totals = [0.0, 0.0]
    for half in range(halves):
        for which, ref in enumerate((gate_ref, up_ref)):
            part = jnp.dot(
                rows, ref[half * wide : (half + 1) * wide], preferred_element_type=F32
            )
            part = jnp.where(spot == half, part, 0.0)
            for shift in range(halves):
                moved = (shift - half) * CAP % part.shape[0]
                totals[which] = totals[which] + (pltpu.roll(part, moved, 0) if moved else part)
    hidden = (totals[0] * sigmoid(totals[0]) * totals[1]).astype(BF16)
    result = jnp.zeros(rows.shape, F32)
    for half in range(halves):
        part = jnp.dot(
            hidden, down_ref[:, half * wide : (half + 1) * wide], preferred_element_type=F32
        )
        result = jnp.where(spot == half, part, result)
    out_ref[...] = result.astype(BF16)


def expert(rows, gate_w, up_w, down_w):
    return pl.pallas_call(
        expert_kernel,
        out_shape=jax.ShapeDtypeStruct(rows.shape, BF16),
        in_specs=vmem_specs(4),
        out_specs=vmem_specs(1)[0],
        cost_estimate=pl.CostEstimate(
            flops=2 * rows.size * gate_w.shape[1] * 3,
            bytes_accessed=6 * gate_w.size,
            transcendentals=0,
        ),
        compiler_params=limit(20),
        name="expert",
    )(rows, gate_w, up_w, down_w)


def combine_kernel(blend_ref, returned_ref, middle_ref, shared_ref, out_ref):
    wide = returned_ref.shape[1]
    returned = returned_ref[...]
    for half in range(blend_ref.shape[0]):
        lanes = slice(half * wide, (half + 1) * wide)
        routed = sum(
            jnp.dot(blend_ref[half, term], returned, preferred_element_type=F32)
            for term in range(blend_ref.shape[1])
        )
        out_ref[:, lanes] = (
            middle_ref[:, lanes] + shared_ref[:, lanes].astype(F32) + routed
        ).astype(BF16)


def combine(blend, returned, middle, shared):
    return pl.pallas_call(
        combine_kernel,
        out_shape=jax.ShapeDtypeStruct(middle.shape, BF16),
        in_specs=vmem_specs(4),
        out_specs=vmem_specs(1)[0],
        compiler_params=limit(8),
        name="combine",
    )(blend, returned, middle, shared)


def per_device(
    residual_input,
    attention_norm_gain,
    receptance_weight,
    key_weight,
    value_weight,
    decay_weight,
    correction_rate_weight,
    output_gate_weight,
    decay_offset,
    correction_rate_offset,
    self_term_weight,
    head_read_gain,
    previous_state,
    attention_output_weight,
    feedforward_norm_gain,
    routes,
    routing_weight,
    routed_gate_weight,
    routed_up_weight,
    routed_down_weight,
    common_gate_weight,
    common_up_weight,
    common_down_weight,
):
    ep_size = lax.axis_size("ep")
    device = lax.axis_index("ep")
    tally = residual_input.shape[0]
    places = ep_size // INNER
    outer = places // MIDDLE

    def flip(array, mask):
        return lax.ppermute(array, "ep", [(s, s ^ mask) for s in range(ep_size)])

    normed, pack = prepare(
        residual_input,
        attention_norm_gain,
        (
            receptance_weight,
            key_weight,
            value_weight,
            decay_weight,
            correction_rate_weight,
            output_gate_weight,
        ),
    )
    side = flip(pack, 2)
    near = flip(pack, 1)
    chunks = [None] * places
    for k in range(outer - 1, -1, -1):
        chunk = normed if k == 0 else flip(normed, INNER * MIDDLE * k)
        chunks[MIDDLE * k] = chunk
        chunks[MIDDLE * k + 1] = flip(chunk, INNER)
    expert_count = routed_gate_weight.shape[0] * ep_size
    own_routes = lax.dynamic_slice_in_dim(routes, device * tally, tally, 0)
    own_weight = lax.dynamic_slice_in_dim(routing_weight, device * tally, tally, 0)
    halves = 8 // CAP
    select, blend = route(own_routes, own_weight, expert_count, halves)

    vectors = jnp.stack(
        [decay_offset, correction_rate_offset, self_term_weight, head_read_gain]
    ).reshape(4, places, LANES)
    side, select, blend, vectors, *chunks = lax.optimization_barrier(
        (side, select, blend, vectors, *chunks)
    )
    packs = [pack, near, side, flip(side, 1)]
    where = jnp.stack([lax.rem(device, INNER), lax.div(device, INNER)]).astype(jnp.int32)
    projected = project(where, chunks, packs)
    projected, vectors = lax.optimization_barrier((projected, vectors))
    projected, vectors = lax.optimization_barrier((projected, linger(vectors, 100_000)))
    groups = [[p * INNER + q for p in range(places)] for q in range(INNER)]
    columns = lax.all_to_all(
        projected, "ep", split_axis=0, concat_axis=0, tiled=True, axis_index_groups=groups
    )

    send, normed_ffn, middle, decay, scaled, update = attend(
        columns,
        vectors,
        previous_state,
        residual_input,
        feedforward_norm_gain,
        select,
        attention_output_weight,
    )
    rows = lax.all_to_all(send, "ep", split_axis=0, concat_axis=0, tiled=True)
    next_state = update_state(previous_state, decay, scaled, update)
    shared = expert_mlp(normed_ffn, common_gate_weight, common_up_weight, common_down_weight)
    output = expert(rows, routed_gate_weight[0], routed_up_weight[0], routed_down_weight[0])
    returned = lax.all_to_all(output, "ep", split_axis=0, concat_axis=0, tiled=True)
    hidden_out = combine(blend, returned, middle, shared)
    return (hidden_out, next_state)


def solution(mesh):
    return jax.shard_map(
        per_device,
        mesh=mesh,
        in_specs=(
            P(("grp", "ep"), None),
            P(),
            P(None, "ep"),
            P(None, "ep"),
            P(None, "ep"),
            P(None, "ep"),
            P(None, "ep"),
            P(None, "ep"),
            P(),
            P(),
            P(),
            P(),
            P(("grp", "ep"), None, None),
            P(),
            P(),
            P("grp", None),
            P("grp", None),
            P("ep", None, None),
            P("ep", None, None),
            P("ep", None, None),
            P(),
            P(),
            P(),
        ),
        out_specs=(P(("grp", "ep"), None), P(("grp", "ep"), None, None)),
        check_vma=False,
    )
```

```python
import functools
import math

import jax
import jax.numpy as jnp
from jax import lax
from jax.experimental import pallas as pl
from jax.experimental.pallas import tpu as pltpu
from jax.sharding import PartitionSpec as P

HEAD_SIZE = 64
LANES = 128
ROLES = 6
CAP = 4
INNER = 4
MIDDLE = 2
UPDATE_PARTS = 4


F32 = jnp.float32
BF16 = jnp.bfloat16
VMEM = pltpu.MemorySpace.VMEM
HBM = pltpu.MemorySpace.HBM
SMEM = pltpu.MemorySpace.SMEM


def vmem_specs(count):
    return [pl.BlockSpec(memory_space=VMEM) for _ in range(count)]


def hbm_specs(count):
    return [pl.BlockSpec(memory_space=HBM) for _ in range(count)]


def limit(mebibytes):
    return pltpu.CompilerParams(vmem_limit_bytes=mebibytes << 20)


def scaled_rows(rows, gain):
    width = gain.shape[1]
    scale = lax.rsqrt(jnp.mean(rows * rows, axis=-1, keepdims=True) + 1e-06)
    parts = [
        rows[:, j * width : (j + 1) * width] * scale * gain[j : j + 1].astype(F32)
        for j in range(gain.shape[0])
    ]
    return jnp.concatenate(parts, axis=1).astype(BF16)


def sigmoid(x):
    return 1.0 / (1.0 + jnp.exp(-x))


def prepare_kernel(residual_hbm, gain_hbm, *refs):
    *weights, normed_ref, packed_ref, residual_ref, gain_ref, sems = refs
    width = weights[0].shape[0]
    copies = [
        pltpu.make_async_copy(residual_hbm, residual_ref, sems.at[0]),
        pltpu.make_async_copy(gain_hbm, gain_ref, sems.at[1]),
    ] + [
        pltpu.make_async_copy(
            ref, packed_ref.at[role * width : (role + 1) * width, :], sems.at[2 + role]
        )
        for role, ref in enumerate(weights)
    ]
    for copy in copies:
        copy.start()
    copies[0].wait()
    copies[1].wait()
    normed_ref[...] = scaled_rows(residual_ref[...].astype(F32), gain_ref[...])
    for copy in copies[2:]:
        copy.wait()


def prepare(residual, gain, weights):
    width, depth = weights[0].shape
    gain = gain.reshape(-1, LANES)
    return pl.pallas_call(
        prepare_kernel,
        out_shape=(
            pltpu.VMEM(residual.shape, BF16),
            pltpu.VMEM((len(weights) * width, depth), BF16),
        ),
        in_specs=hbm_specs(2 + len(weights)),
        out_specs=tuple(vmem_specs(2)),
        scratch_shapes=[
            pltpu.VMEM(residual.shape, BF16),
            pltpu.VMEM(gain.shape, BF16),
            pltpu.SemaphoreType.DMA((2 + len(weights),)),
        ],
        compiler_params=limit(60),
        name="prepare",
    )(residual, gain, *weights)


def project_kernel(places, device_ref, *refs):
    chunks = refs[:places]
    leads = refs[places : places + INNER]
    packs = refs[places + INNER : places + 2 * INNER]
    out_ref, rows_ref, weight_ref, row_sems, weight_sems = refs[places + 2 * INNER :]
    width = leads[0].shape[0]
    tally = out_ref.shape[1]
    lane_place, row_place = lax.rem(device_ref[0], INNER), lax.div(device_ref[0], INNER)
    row_copies = [
        pltpu.make_async_copy(ref, rows_ref.at[near], row_sems.at[near])
        for near, ref in enumerate(chunks)
    ]
    weight_copies = []
    for role in range(ROLES):
        for near in range(INNER):
            spot = jnp.bitwise_xor(lane_place, near)
            start = pl.multiple_of((role * INNER + spot) * width, width)
            source = packs[near].at[(role - 1) * width : role * width, :] if role else leads[near]
            weight_copies.append(
                pltpu.make_async_copy(
                    source,
                    weight_ref.at[pl.ds(start, width), :],
                    weight_sems.at[role, near],
                )
            )
    for copy in row_copies + weight_copies:
        copy.start()
    for copy in row_copies:
        copy.wait()
    rows = jnp.concatenate([rows_ref[k].astype(F32) for k in range(places)], axis=0).astype(BF16)
    for copy in weight_copies:
        copy.wait()
    result = lax.dot_general(
        rows, weight_ref[...], (((1,), (1,)), ((), ())), preferred_element_type=F32
    )
    for near in range(places):
        out_ref[jnp.bitwise_xor(row_place, near)] = result[
            near * tally : (near + 1) * tally
        ].astype(BF16)


def project(device, chunks, leads, packs):
    places = len(chunks)
    tally, depth = chunks[0].shape
    rows = leads[0].shape[0] * INNER * ROLES
    return pl.pallas_call(
        functools.partial(project_kernel, places),
        out_shape=pltpu.VMEM((places, tally, rows), BF16),
        in_specs=[pl.BlockSpec(memory_space=SMEM)]
        + hbm_specs(places + 2 * INNER),
        out_specs=vmem_specs(1)[0],
        scratch_shapes=[
            pltpu.VMEM((places, tally, depth), BF16),
            pltpu.VMEM((rows, depth), BF16),
            pltpu.SemaphoreType.DMA((places,)),
            pltpu.SemaphoreType.DMA((ROLES, INNER)),
        ],
        cost_estimate=pl.CostEstimate(
            flops=2 * places * tally * rows * depth,
            bytes_accessed=2 * rows * depth,
            transcendentals=0,
        ),
        compiler_params=limit(60),
        name="project",
    )(device, *chunks, *leads, *packs)


def linger_kernel(in_ref, out_ref):
    out_ref[...] = in_ref[...]


def linger(array, nanoseconds):
    return pl.pallas_call(
        linger_kernel,
        out_shape=jax.ShapeDtypeStruct(array.shape, array.dtype),
        in_specs=vmem_specs(1),
        out_specs=vmem_specs(1)[0],
        cost_estimate=pl.CostEstimate(
            flops=nanoseconds * 500_000, bytes_accessed=0, transcendentals=0
        ),
        compiler_params=limit(1),
        name="linger",
    )(array)


def route_kernel(device_ref, routes_ref, weight_ref, select_ref, blend_ref):
    halves, slots, tally = select_ref.shape
    top, tokens = routes_ref.shape
    shift = lax.rem(tokens - device_ref[0] * tally, tokens)
    turned = pltpu.roll(routes_ref[...], shift, 1)[:, :LANES]
    weights = pltpu.roll(weight_ref[...], shift, 1)[:, :LANES]
    same = lax.broadcasted_iota(jnp.int32, (tally, LANES), 0) == lax.broadcasted_iota(
        jnp.int32, (tally, LANES), 1
    )

    def upright(array):
        return lax.dot_general(
            same.astype(F32),
            array.astype(F32),
            (((1,), (1,)), ((), ())),
            preferred_element_type=F32,
            precision=lax.Precision.HIGHEST,
        )

    routes = upright(turned).astype(jnp.int32)
    weights = upright(weights)
    chunk = halves * CAP
    lane = lax.broadcasted_iota(jnp.int32, (tally, slots), 1)
    hit = jnp.zeros((tally, slots), F32)
    weight = jnp.zeros((tally, slots), F32)
    for j in range(top):
        match = routes[:, j : j + 1] == lax.div(lane, chunk)
        hit = jnp.where(match, 1.0, hit)
        weight = weight + jnp.where(match, weights[:, j : j + 1], 0.0)
    row = lax.broadcasted_iota(jnp.int32, (tally, tally), 0)
    column = lax.broadcasted_iota(jnp.int32, (tally, tally), 1)
    rank = jnp.dot((column < row).astype(F32), hit, preferred_element_type=F32)
    chosen = (hit > 0.5) & (rank.astype(jnp.int32) == lax.rem(lane, CAP))
    for half in range(halves):
        here = chosen & (lax.rem(lax.div(lane, CAP), halves) == half)
        blend = jnp.where(here, weight, 0.0)
        coarse = blend.astype(BF16)
        blend_ref[half, 0] = coarse
        blend_ref[half, 1] = (blend - coarse.astype(F32)).astype(BF16)
    slot = lax.broadcasted_iota(jnp.int32, (slots, tally), 0)
    hit = jnp.zeros((slots, tally), F32)
    for j in range(top):
        hit = jnp.where(turned[j : j + 1, :tally] == lax.div(slot, chunk), 1.0, hit)
    rank = jnp.dot(hit, (row < column).astype(F32), preferred_element_type=F32)
    chosen = (hit > 0.5) & (rank.astype(jnp.int32) == lax.rem(slot, CAP))
    for half in range(halves):
        here = chosen & (lax.rem(lax.div(slot, CAP), halves) == half)
        select_ref[half] = jnp.where(here, 1.0, 0.0).astype(BF16)


def route(device, routes, weight, tally, experts, halves):
    slots = experts * CAP * halves
    return pl.pallas_call(
        route_kernel,
        out_shape=(
            jax.ShapeDtypeStruct((halves, slots, tally), BF16),
            jax.ShapeDtypeStruct((halves, 2, tally, slots), BF16),
        ),
        in_specs=[pl.BlockSpec(memory_space=SMEM)] + vmem_specs(2),
        out_specs=tuple(vmem_specs(2)),
        compiler_params=limit(60),
        name="route",
    )(device, routes.T, weight.T)


def segment_sum(values):
    row = lax.broadcasted_iota(jnp.int32, (LANES, LANES), 0)
    column = lax.broadcasted_iota(jnp.int32, (LANES, LANES), 1)
    ones = (lax.div(row, HEAD_SIZE) == lax.div(column, HEAD_SIZE)).astype(F32)
    return jnp.dot(values, ones, preferred_element_type=F32, precision=lax.Precision.HIGHEST)


def join(first, first_half, second, second_half):
    lane = lax.broadcasted_iota(jnp.int32, first.shape, 1)
    low = first if first_half == 0 else pltpu.roll(first, HEAD_SIZE, 1)
    high = second if second_half == 1 else pltpu.roll(second, HEAD_SIZE, 1)
    return jnp.where(lane < HEAD_SIZE, low, high)


def spread_heads(parts):
    count = len(parts)
    return [
        join(parts[j // 2], j % 2, parts[count // 2 + j // 2], j % 2) for j in range(count)
    ]


def pair_heads(parts):
    count = len(parts)
    return [
        join(
            parts[2 * b % count],
            2 * b // count,
            parts[(2 * b + 1) % count],
            (2 * b + 1) // count,
        )
        for b in range(count)
    ]


def attend_kernel(
    mixed_cols_ref,
    decay_offset_ref,
    rate_offset_ref,
    self_weight_ref,
    read_gain_ref,
    state_ref,
    residual_ref,
    gain_ref,
    select_ref,
    weight_ref,
    send_ref,
    ffn_ref,
    middle_ref,
    decay_ref,
    scaled_ref,
    update_ref,
    unit_ref,
    faded_ref,
    norm_ref,
    value_ref,
    gate_ref,
    own_ref,
    dot_ref,
    recall_ref,
    read_ref,
    square_ref,
    cross_ref,
    self_ref,
    product_ref,
    ones_ref,
    mixed_ref,
):
    blocks, tally, _ = mixed_cols_ref.shape
    _, heads, width = state_ref.shape
    tiles = width // LANES
    per_step = product_ref.shape[0] // (2 * heads)
    steps = tally // per_step

    row = lax.broadcasted_iota(jnp.int32, ones_ref.shape, 0)
    column = lax.broadcasted_iota(jnp.int32, ones_ref.shape, 1)
    same = lax.div(row, HEAD_SIZE) == lax.rem(column, HEAD_SIZE)
    ones_ref[...] = same.astype(F32).astype(BF16)
    for b in range(blocks):
        rows = pl.ds(b * tally, tally)

        def part(role):
            return mixed_cols_ref[b, :, role * LANES : (role + 1) * LANES].astype(F32)

        def vector(ref):
            return ref[b : b + 1, :]

        receptance, key, value = part(0), part(1), part(2)
        decay = jnp.exp(-math.exp(-0.5) * sigmoid(vector(decay_offset_ref) + part(3)))
        rate = sigmoid(vector(rate_offset_ref) + part(4))
        scaled = key * rate
        cross = receptance * scaled
        faded = decay * receptance
        square_ref[rows, :] = key * key
        cross_ref[rows, :] = cross
        self_ref[rows, :] = cross * vector(self_weight_ref)
        value_ref[rows, :] = value
        gate_ref[rows, :] = sigmoid(part(5))
        for h in range(2):
            wide = pl.ds((2 * b + h) * tally, tally)
            decay_ref[wide, :] = join(decay, h, decay, h)
            scaled_ref[wide, :] = join(scaled, h, scaled, h)
            faded_ref[wide, :] = join(faded, h, faded, h)
    norm = lax.rsqrt(1.0 + segment_sum(square_ref[...]))
    norm_ref[...] = norm
    for b in range(blocks):
        rows = slice(b * tally, (b + 1) * tally)
        key = mixed_cols_ref[b, :, LANES : 2 * LANES].astype(F32)
        unit = key * norm[rows]
        for h in range(2):
            unit_ref[pl.ds((2 * b + h) * tally, tally), :] = join(unit, h, unit, h)
    dot_ref[...] = segment_sum(cross_ref[...])
    own_ref[...] = segment_sum(self_ref[...])

    first = lax.broadcasted_iota(jnp.int32, (blocks, LANES), 1) < HEAD_SIZE

    def step_tokens(step, carry):
        def token(i, carry):
            spot = step * per_step + i
            source = pl.ds(spot, heads, stride=tally)
            unit, faded = unit_ref[source, :], faded_ref[source, :]
            row = pl.multiple_of(2 * heads * i, 2 * heads)
            for tile in range(tiles):
                lanes = slice(tile * LANES, (tile + 1) * LANES)
                state = state_ref[spot, :, lanes]
                product_ref[pl.ds(row, heads), lanes] = (state * unit).astype(BF16)
                product_ref[pl.ds(row + heads, heads), lanes] = (state * faded).astype(BF16)
            return carry

        lax.fori_loop(0, per_step, token, 0)
        sums = jnp.dot(product_ref[...], ones_ref[...], preferred_element_type=F32)
        for i in range(per_step):
            at = pl.ds(step * per_step + i, blocks, stride=tally)
            for which, ref in enumerate((recall_ref, read_ref)):
                row = (2 * i + which) * heads
                ref[at, :] = jnp.where(
                    first, sums[row : row + blocks], sums[row + blocks : row + heads]
                )
        return carry

    lax.fori_loop(0, steps, step_tokens, 0)

    def blockwise(array):
        return [array[b * tally : (b + 1) * tally] for b in range(blocks)]

    recall = jnp.concatenate(pair_heads(blockwise(recall_ref[...])), axis=0)
    read = jnp.concatenate(pair_heads(blockwise(read_ref[...])), axis=0)
    update = value_ref[...] - recall * norm_ref[...]
    for j, part in enumerate(spread_heads(blockwise(update))):
        update_ref[j * tally : (j + 1) * tally, :] = part
    read = read + update * dot_ref[...]
    centered = read - segment_sum(read) * (1.0 / HEAD_SIZE)
    variance = segment_sum(centered * centered) * (1.0 / HEAD_SIZE)
    normal = centered * lax.rsqrt(variance + 0.00064)
    own = own_ref[...] * value_ref[...]
    gate = gate_ref[...]
    for b in range(blocks):
        rows = slice(b * tally, (b + 1) * tally)
        mixed_ref[:, b * LANES : (b + 1) * LANES] = (
            (normal[rows] * read_gain_ref[b : b + 1, :] + own[rows]) * gate[rows]
        ).astype(BF16)
    attended = jnp.dot(mixed_ref[...], weight_ref[...], preferred_element_type=F32)
    middle = residual_ref[...].astype(F32) + attended.astype(BF16).astype(F32)
    middle_ref[...] = middle
    ffn = scaled_rows(middle, gain_ref[...])
    ffn_ref[...] = ffn
    halves = select_ref.shape[0]
    wide = ffn.shape[1] // halves
    send_ref[...] = sum(
        jnp.dot(
            select_ref[half],
            ffn[:, half * wide : (half + 1) * wide],
            preferred_element_type=F32,
        )
        for half in range(halves)
    ).astype(BF16)


def attend(columns, vectors, state, residual, gain, select, output_weight):
    blocks, tally, _ = columns.shape
    depth = residual.shape[1]
    halves, slots, _ = select.shape
    rows = blocks * tally
    per_step = tally // 2 if tally % 2 == 0 else tally
    flat = jax.ShapeDtypeStruct((rows, LANES), F32)
    wide = jax.ShapeDtypeStruct((2 * rows, LANES), F32)
    return pl.pallas_call(
        attend_kernel,
        out_shape=(
            jax.ShapeDtypeStruct((slots, depth // halves), BF16),
            jax.ShapeDtypeStruct((tally, depth), BF16),
            jax.ShapeDtypeStruct((tally, depth), F32),
            wide,
            wide,
            flat,
        ),
        in_specs=vmem_specs(10),
        out_specs=tuple(vmem_specs(6)),
        scratch_shapes=[pltpu.VMEM((2 * rows, LANES), F32) for _ in range(2)]
        + [pltpu.VMEM((rows, LANES), F32) for _ in range(10)]
        + [
            pltpu.VMEM((2 * per_step * state.shape[1], state.shape[2]), BF16),
            pltpu.VMEM((state.shape[2], LANES), BF16),
            pltpu.VMEM((tally, blocks * LANES), BF16),
        ],
        cost_estimate=pl.CostEstimate(
            flops=8 * state.size, bytes_accessed=4 * state.size, transcendentals=0
        ),
        compiler_params=limit(28),
        name="attend",
    )(columns, *vectors, state, residual, gain.reshape(-1, LANES), select, output_weight)


def update_kernel(state_ref, decay_ref, scaled_ref, update_ref, out_ref, terms_ref):
    step = pl.program_id(0)
    tally, heads, part = state_ref.shape
    blocks = heads // 2
    first = lax.broadcasted_iota(jnp.int32, (blocks, LANES), 1) < HEAD_SIZE

    @pl.when(step == 0)
    def _():
        for i in range(tally):
            update = update_ref[pl.ds(i, blocks, stride=tally), :]
            coarse = update.astype(BF16).astype(F32)
            fine = update - coarse
            low = jnp.where(first, coarse, pltpu.roll(fine, HEAD_SIZE, 1))
            high = jnp.where(first, pltpu.roll(coarse, HEAD_SIZE, 1), fine)
            terms_ref[i * heads : (i + 1) * heads, :] = jnp.concatenate(
                [low, high], axis=0
            ).astype(BF16)

    row = lax.broadcasted_iota(jnp.int32, (LANES, part), 0)
    column = lax.broadcasted_iota(jnp.int32, (LANES, part), 1) + step * part
    same = lax.rem(row, HEAD_SIZE) == lax.div(column, HEAD_SIZE)
    spread = jnp.dot(
        terms_ref[...], same.astype(F32).astype(BF16), preferred_element_type=F32
    )
    for i in range(tally):
        source = pl.ds(i, heads, stride=tally)
        decay, scaled = decay_ref[source, :], scaled_ref[source, :]
        for j in range(part // LANES):
            lanes = slice(j * LANES, (j + 1) * LANES)
            out_ref[i, :, lanes] = (
                state_ref[i, :, lanes] * decay
                + spread[i * heads : (i + 1) * heads, lanes] * scaled
            )


def update_state(state, decay, scaled, update):
    tally, heads, width = state.shape
    wide = pl.BlockSpec(decay.shape, lambda i: (0, 0))
    flat = pl.BlockSpec(update.shape, lambda i: (0, 0))
    block = pl.BlockSpec((tally, heads, width // UPDATE_PARTS), lambda i: (0, 0, i))
    return pl.pallas_call(
        update_kernel,
        grid=(UPDATE_PARTS,),
        out_shape=jax.ShapeDtypeStruct(state.shape, F32),
        in_specs=[block, wide, wide, flat],
        out_specs=block,
        scratch_shapes=[pltpu.VMEM((tally * heads, LANES), BF16)],
        cost_estimate=pl.CostEstimate(
            flops=3 * state.size, bytes_accessed=8 * state.size, transcendentals=0
        ),
        compiler_params=limit(60),
        name="update_state",
    )(state, decay, scaled, update)


def expert_mlp(rows, gate_w, up_w, down_w):
    gate = jnp.dot(rows, gate_w, preferred_element_type=F32)
    upward = jnp.dot(rows, up_w, preferred_element_type=F32)
    hidden = (jax.nn.silu(gate) * upward).astype(BF16)
    return jnp.dot(hidden, down_w, preferred_element_type=F32).astype(BF16)


def expert_kernel(rows_ref, gate_ref, up_ref, down_ref, out_ref):
    wide = rows_ref.shape[1]
    halves = gate_ref.shape[0] // wide
    rows = rows_ref[...]
    spot = lax.rem(
        lax.div(lax.broadcasted_iota(jnp.int32, (rows.shape[0], 1), 0), CAP), halves
    )
    totals = [0.0, 0.0]
    for half in range(halves):
        for which, ref in enumerate((gate_ref, up_ref)):
            part = jnp.dot(
                rows, ref[half * wide : (half + 1) * wide], preferred_element_type=F32
            )
            part = jnp.where(spot == half, part, 0.0)
            for shift in range(halves):
                moved = (shift - half) * CAP % part.shape[0]
                totals[which] = totals[which] + (pltpu.roll(part, moved, 0) if moved else part)
    hidden = (totals[0] * sigmoid(totals[0]) * totals[1]).astype(BF16)
    result = jnp.zeros(rows.shape, F32)
    for half in range(halves):
        part = jnp.dot(
            hidden, down_ref[:, half * wide : (half + 1) * wide], preferred_element_type=F32
        )
        result = jnp.where(spot == half, part, result)
    out_ref[...] = result.astype(BF16)


def expert(rows, gate_w, up_w, down_w):
    return pl.pallas_call(
        expert_kernel,
        out_shape=jax.ShapeDtypeStruct(rows.shape, BF16),
        in_specs=vmem_specs(4),
        out_specs=vmem_specs(1)[0],
        cost_estimate=pl.CostEstimate(
            flops=2 * rows.size * gate_w.shape[1] * 3,
            bytes_accessed=6 * gate_w.size,
            transcendentals=0,
        ),
        compiler_params=limit(20),
        name="expert",
    )(rows, gate_w, up_w, down_w)


def combine_kernel(blend_ref, returned_ref, middle_ref, shared_ref, out_ref):
    wide = returned_ref.shape[1]
    returned = returned_ref[...]
    for half in range(blend_ref.shape[0]):
        lanes = slice(half * wide, (half + 1) * wide)
        routed = sum(
            jnp.dot(blend_ref[half, term], returned, preferred_element_type=F32)
            for term in range(blend_ref.shape[1])
        )
        out_ref[:, lanes] = (
            middle_ref[:, lanes] + shared_ref[:, lanes].astype(F32) + routed
        ).astype(BF16)


def combine(blend, returned, middle, shared):
    return pl.pallas_call(
        combine_kernel,
        out_shape=jax.ShapeDtypeStruct(middle.shape, BF16),
        in_specs=vmem_specs(4),
        out_specs=vmem_specs(1)[0],
        compiler_params=limit(8),
        name="combine",
    )(blend, returned, middle, shared)


def per_device(
    residual_input,
    attention_norm_gain,
    receptance_weight,
    key_weight,
    value_weight,
    decay_weight,
    correction_rate_weight,
    output_gate_weight,
    decay_offset,
    correction_rate_offset,
    self_term_weight,
    head_read_gain,
    previous_state,
    attention_output_weight,
    feedforward_norm_gain,
    routes,
    routing_weight,
    routed_gate_weight,
    routed_up_weight,
    routed_down_weight,
    common_gate_weight,
    common_up_weight,
    common_down_weight,
):
    ep_size = lax.axis_size("ep")
    device = lax.axis_index("ep")
    tally = residual_input.shape[0]
    places = ep_size // INNER
    outer = places // MIDDLE

    def flip(array, mask):
        return lax.ppermute(array, "ep", [(s, s ^ mask) for s in range(ep_size)])

    where = device.astype(jnp.int32).reshape(1)
    lead, *weights = [
        weight.T
        for weight in (
            receptance_weight,
            key_weight,
            value_weight,
            decay_weight,
            correction_rate_weight,
            output_gate_weight,
        )
    ]
    lead_side = flip(lead, 2)
    normed, pack = prepare(residual_input, attention_norm_gain, weights)
    side = flip(pack, 2)
    chunks = [None] * places
    for k in range(outer - 1, -1, -1):
        chunk = normed if k == 0 else flip(normed, INNER * MIDDLE * k)
        chunks[MIDDLE * k] = chunk
        chunks[MIDDLE * k + 1] = flip(chunk, INNER)
    halves = 8 // CAP
    experts = routed_gate_weight.shape[0] * ep_size
    select, blend = route(where, routes, routing_weight, tally, experts, halves)
    side, select, blend, *near = lax.optimization_barrier(
        (side, select, blend, *chunks[::MIDDLE])
    )
    chunks[::MIDDLE] = near
    leads = [lead, flip(lead, 1), lead_side, flip(lead_side, 1)]
    packs = [pack, flip(pack, 1), side, flip(side, 1)]
    vectors = [
        vector.reshape(places, LANES)
        for vector in (decay_offset, correction_rate_offset, self_term_weight, head_read_gain)
    ]
    projected = project(where, chunks, leads, packs)
    projected, offset = lax.optimization_barrier((projected, vectors[0]))
    projected, vectors[0] = lax.optimization_barrier((projected, linger(offset, 100_000)))
    groups = [[p * INNER + q for p in range(places)] for q in range(INNER)]
    columns = lax.all_to_all(
        projected, "ep", split_axis=0, concat_axis=0, tiled=True, axis_index_groups=groups
    )
    send, normed_ffn, middle, decay, scaled, update = attend(
        columns,
        vectors,
        previous_state,
        residual_input,
        feedforward_norm_gain,
        select,
        attention_output_weight,
    )
    rows = lax.all_to_all(send, "ep", split_axis=0, concat_axis=0, tiled=True)
    next_state = update_state(previous_state, decay, scaled, update)
    shared = expert_mlp(normed_ffn, common_gate_weight, common_up_weight, common_down_weight)
    output = expert(rows, routed_gate_weight[0], routed_up_weight[0], routed_down_weight[0])
    returned = lax.all_to_all(output, "ep", split_axis=0, concat_axis=0, tiled=True)
    hidden_out = combine(blend, returned, middle, shared)
    return (hidden_out, next_state)


def solution(mesh):
    return jax.shard_map(
        per_device,
        mesh=mesh,
        in_specs=(
            P(("grp", "ep"), None),
            P(),
            P(None, "ep"),
            P(None, "ep"),
            P(None, "ep"),
            P(None, "ep"),
            P(None, "ep"),
            P(None, "ep"),
            P(),
            P(),
            P(),
            P(),
            P(("grp", "ep"), None, None),
            P(),
            P(),
            P("grp", None),
            P("grp", None),
            P("ep", None, None),
            P("ep", None, None),
            P("ep", None, None),
            P(),
            P(),
            P(),
        ),
        out_specs=(P(("grp", "ep"), None), P(("grp", "ep"), None, None)),
        check_vma=False,
    )
```
